32 devices in a mesh: rep: 2 (over x), fs: 8 (over z, y), tp: 2 (over core).
Axes of the slice: x: 2, y: 2, z: 4, core: 2. Of those that a mesh axis runs over, the one named last changes fastest.
Arguments:
- tokens: bfloat16 [16, 384, 2048], P(('rep', 'fs')), may hold values from -6 to 6
- mix_gain: float32 [2048], replicated, may hold values from 0.1 to 1.9
- value_weight: float32 [2048, 2048], P('fs', 'tp'), may hold values from -0.125 to 0.125
- value_scale: float32 [2048], P(('tp', 'fs')), may hold values from 0.5 to 2
- inner_weight: float32 [2048, 2048], P('fs', 'tp'), may hold values from -0.125 to 0.125
- inner_scale: float32 [2048], P(('tp', 'fs')), may hold values from 0.5 to 2
- outer_weight: float32 [2048, 2048], P('fs', 'tp'), may hold values from -0.125 to 0.125
- outer_scale: float32 [2048], P(('tp', 'fs')), may hold values from 0.5 to 2
- conv_taps: float32 [3, 2048], P(None, 'tp'), may hold values from -3 to 3
- out_weight: float32 [2048, 2048], P('tp', 'fs'), may hold values from -0.125 to 0.125
- out_scale: float32 [2048], P('fs'), may hold values from 0.5 to 2
- mlp_gain: float32 [2048], replicated, may hold values from 0.1 to 1.9
- up_weight: float32 [2048, 6144], P('fs', 'tp'), may hold values from -0.125 to 0.125
- up_scale: float32 [6144], P(('tp', 'fs')), may hold values from 0.5 to 2
- down_weight: float32 [6144, 2048], P('tp', 'fs'), may hold values from -0.078125 to 0.078125
- down_scale: float32 [2048], P('fs'), may hold values from 0.5 to 2
Outputs:
- layer_out: bfloat16 [16, 384, 2048], P(('rep', 'fs'))
The draws below stay inside these ranges and needn't reach their ends.
All inputs are finite; a program needn't handle non-finite values.
Results may differ from the reference program's by a relative error of at most 0.02.
Values may be sent and summed in bfloat16 or wider, within the bound.
No kernel may reach another device: no remote copies, remote signals or barrier semaphores. Data moves between devices by JAX's collectives and lax.ppermute only.
A program may use at most 128 MiB of HBM per device.

```python
import math
import jax
import jax.numpy as jnp
from jax import lax

D = 2048
FF = 6144
TOK_DEV = 384
SEQS = 16
N_TP = 2


def block_scale(rng, dims, shards, low, high):
    def one(axis_at, shards_of):
        heights = jax.random.uniform(jax.random.fold_in(jax.random.fold_in(rng, 6), axis_at), (shards_of,), jnp.float32, low / len(shards), high / len(shards))
        return jnp.repeat(jnp.exp(heights), dims[axis_at] // shards_of).reshape((-1,) + (1,) * (len(dims) - axis_at - 1))

    level = one(*shards[0])
    for cut in shards[1:]:
        level = level * one(*cut)
    return level


def scatter_about(key, shape, scale, limit, cuts=(), kind=jnp.bfloat16):
    values = scale * jax.random.normal(key, shape, jnp.float32)
    if cuts:
        values = values * block_scale(key, shape, cuts, -0.22, 0.18)
    return jnp.clip(values, -limit, limit).astype(kind)


def setup_inputs(seed: int = 0) -> dict:
    key_of = jax.random.split(jax.random.key(seed), 17)
    return {
        "tokens": scatter_about(key_of[0], (SEQS, TOK_DEV, D), 1.0, 6.0, ((0, 16),)),
        "mix_gain": jnp.clip(1.0 + 0.18 * jax.random.normal(key_of[1], (D,), jnp.float32), 0.1, 1.9),
        "value_weight": scatter_about(key_of[2], (D, D), D ** -0.5, 0.125, ((0, 8), (1, 2)), jnp.float32),
        "value_scale": jnp.clip(jnp.exp(math.log(2.0) - 1.3862944 * jax.random.uniform(key_of[3], (D,), jnp.float32) ** block_scale(key_of[3], (D,), ((0, 16),), -0.2, 0.2)), 0.5, 2.0),
        "inner_weight": scatter_about(key_of[4], (D, D), D ** -0.5, 0.125, ((0, 8), (1, 2)), jnp.float32),
        "inner_scale": jnp.clip(jnp.exp(math.log(2.0) - 1.3862944 * jax.random.uniform(key_of[5], (D,), jnp.float32) ** block_scale(key_of[5], (D,), ((0, 16),), -0.2, 0.2)), 0.5, 2.0),
        "outer_weight": scatter_about(key_of[6], (D, D), D ** -0.5, 0.125, ((0, 8), (1, 2)), jnp.float32),
        "outer_scale": jnp.clip(jnp.exp(math.log(2.0) - 1.3862944 * jax.random.uniform(key_of[7], (D,), jnp.float32) ** block_scale(key_of[7], (D,), ((0, 16),), -0.2, 0.2)), 0.5, 2.0),
        "conv_taps": scatter_about(key_of[8], (3, D), 0.6, 3.0, ((1, 2),), jnp.float32),
        "out_weight": scatter_about(key_of[9], (D, D), D ** -0.5, 0.125, ((0, 2), (1, 8)), jnp.float32),
        "out_scale": jnp.clip(jnp.exp(math.log(2.0) - 1.3862944 * jax.random.uniform(key_of[10], (D,), jnp.float32) ** block_scale(key_of[10], (D,), ((0, 8),), -0.2, 0.2)), 0.5, 2.0),
        "mlp_gain": jnp.clip(1.0 + 0.18 * jax.random.normal(key_of[11], (D,), jnp.float32), 0.1, 1.9),
        "up_weight": scatter_about(key_of[12], (D, FF), D ** -0.5, 0.125, ((0, 8), (1, 2)), jnp.float32),
        "up_scale": jnp.clip(jnp.exp(math.log(2.0) - 1.3862944 * jax.random.uniform(key_of[13], (FF,), jnp.float32) ** block_scale(key_of[13], (FF,), ((0, 16),), -0.2, 0.2)), 0.5, 2.0),
        "down_weight": scatter_about(key_of[14], (FF, D), FF ** -0.5, 0.078125, ((0, 2), (1, 8)), jnp.float32),
        "down_scale": jnp.clip(jnp.exp(math.log(2.0) - 1.3862944 * jax.random.uniform(key_of[15], (D,), jnp.float32) ** block_scale(key_of[15], (D,), ((0, 8),), -0.2, 0.2)), 0.5, 2.0),
    }


norm_eps = 1e-06

def normalize(values, gain):
    return values * lax.rsqrt(lax.optimization_barrier(jnp.mean(values * values, axis=-1, keepdims=True)) + norm_eps) * gain

def block_sum(left, right, blocks):
    rows = left.shape[0]
    width = left.shape[1] // blocks
    left_blocks = left.reshape(rows, blocks, width).astype(jnp.float32)
    right_blocks = right.reshape(blocks, width, right.shape[1]).astype(jnp.float32)
    parts = jnp.einsum('lnk,nkd->nld', left_blocks, right_blocks).astype(jnp.bfloat16)
    parts = lax.optimization_barrier(parts)
    return lax.optimization_barrier(jnp.sum(parts.astype(jnp.float32), axis=0))

def reference(tokens, mix_gain, value_weight, value_scale, inner_weight, inner_scale, outer_weight, outer_scale, conv_taps, out_weight, out_scale, mlp_gain, up_weight, up_scale, down_weight, down_scale):
    value_b = value_weight.astype(jnp.bfloat16)
    inner_b = inner_weight.astype(jnp.bfloat16)
    outer_b = outer_weight.astype(jnp.bfloat16)
    out_b = out_weight.astype(jnp.bfloat16)
    up_b = up_weight.astype(jnp.bfloat16)
    down_b = down_weight.astype(jnp.bfloat16)

    def one_sequence(sequence):
        start = sequence.astype(jnp.float32)
        normed = normalize(start, mix_gain).astype(jnp.bfloat16)
        value = jnp.dot(normed, value_b, preferred_element_type=jnp.float32) * value_scale
        inner = jnp.dot(normed, inner_b, preferred_element_type=jnp.float32) * inner_scale
        outer = jnp.dot(normed, outer_b, preferred_element_type=jnp.float32) * outer_scale
        gated = inner * value
        padded = jnp.pad(gated, ((1, 1), (0, 0)))
        conv = conv_taps[0] * padded[:-2] + conv_taps[1] * padded[1:-1] + conv_taps[2] * padded[2:]
        hidden = (outer * conv).astype(jnp.bfloat16)
        middle = start + block_sum(hidden, out_b, N_TP) * out_scale
        normed_mid = normalize(middle, mlp_gain).astype(jnp.bfloat16)
        upper = jnp.dot(normed_mid, up_b, preferred_element_type=jnp.float32) * up_scale
        act = jnp.square(jax.nn.relu(upper)).astype(jnp.bfloat16)
        return (middle + block_sum(act, down_b, N_TP) * down_scale).astype(jnp.bfloat16)
    return lax.map(one_sequence, tokens)
```

```python
import jax
import jax.numpy as jnp
from jax import lax
from jax.sharding import PartitionSpec as P

norm_eps = 1e-06
bf16 = jnp.bfloat16
f32 = jnp.float32


def normalize(values, gain):
    return values * lax.rsqrt(jnp.mean(values * values, axis=-1, keepdims=True) + norm_eps) * gain


def dot(left, right):
    return jnp.dot(left, right, preferred_element_type=f32)


def cut(array, index, width, axis):
    return lax.dynamic_slice_in_dim(array, index * width, width, axis)


def body(
    tokens,
    mix_gain,
    value_weight,
    value_scale,
    inner_weight,
    inner_scale,
    outer_weight,
    outer_scale,
    conv_taps,
    out_weight,
    out_scale,
    mlp_gain,
    up_weight,
    up_scale,
    down_weight,
    down_scale,
):
    R, F, N = lax.axis_size("rep"), lax.axis_size("fs"), lax.axis_size("tp")
    B = 2
    A = F // B
    r, f, c = lax.axis_index("rep"), lax.axis_index("fs"), lax.axis_index("tp")
    z, y = f // B, f % B
    q = r * B + y
    Q = R * B
    T, D = tokens.shape[1:]
    rows = T // N
    peers = [(dr, dy) for dr in range(R) for dy in range(B)]

    def fs_perm(dz, dy):
        return [(i, ((i // B + dz) % A) * B + (i % B + dy) % B) for i in range(F)]

    def to_fs(array, dz, dy):
        return lax.ppermute(array, "fs", fs_perm(dz, dy))

    def to_peer(array, dr, dy):
        perm = [
            (k * F + i, ((k + dr) % R) * F + (i // B) * B + (i % B + dy) % B)
            for k in range(R)
            for i in range(F)
        ]
        return lax.ppermute(array, ("rep", "fs"), perm)

    def to_core(array, dc):
        return lax.ppermute(array, "tp", [(i, (i + dc) % N) for i in range(N)])

    def ring(piece):
        pieces = [piece]
        for _ in range(A - 1):
            pieces.append(to_fs(pieces[-1], 1, 0))
        return pieces

    def quarter(weights, axis, dy):
        index = r * B + (y + dy) % B
        parts = [cut(w, index, w.shape[axis] // Q, axis) for w in weights]
        return jnp.concatenate(parts, axis=1).astype(bf16)

    def gather_relative(weights, axis):
        return [
            ring(quarter(weights, axis, 0) if dy == 0 else to_fs(quarter(weights, axis, dy), 0, dy))
            for dy in range(B)
        ]

    def gather_natural(weight, axis):
        mine = [quarter([weight], axis, 0)]
        for dy in range(1, B):
            mine.append(to_fs(quarter([weight], axis, dy), 0, dy))
        chains = []
        for j in range(B):
            piece = mine[0]
            for dy in range(1, B):
                piece = jnp.where((y - dy) % B == j, mine[dy], piece)
            chains.append(ring(piece))
        return chains

    start = tokens[0].astype(f32)
    start_rows = cut(start, c, rows, 0)
    normed_own = normalize(start_rows, mix_gain).astype(bf16)

    def spread(own):
        seqs = [own if j == 0 else to_peer(own, *peers[j]) for j in range(Q)]
        if N > 2:
            every = lax.all_gather(jnp.concatenate(seqs, axis=0), "tp", axis=0)
            return jnp.take(every, (c - jnp.arange(N)) % N, axis=0).reshape(-1, D)
        halves = [seqs] + [[to_core(s, dc) for s in seqs] for dc in range(1, N)]
        return jnp.concatenate([s for half in halves for s in half], axis=0)

    vio = gather_relative([value_weight, inner_weight, outer_weight], 1)
    normed = spread(normed_own)

    smalls = jnp.concatenate(
        [value_scale, inner_scale, outer_scale, up_scale, out_scale, down_scale]
    )
    both = jnp.stack([smalls, to_fs(smalls, 0, 1)])
    both = jnp.where(y == 0, both, both[::-1])
    small_ring = jnp.stack(ring(both))
    small_nat = jnp.concatenate(
        [lax.dynamic_index_in_dim(small_ring, (z - zz) % A, 0) for zz in range(A)], axis=0
    ).reshape(F, -1)
    w0 = value_scale.shape[0]
    w1 = up_scale.shape[0]
    w2 = out_scale.shape[0]
    offs = [0, w0, 2 * w0, 3 * w0, 3 * w0 + w1, 3 * w0 + w1 + w2, 3 * w0 + w1 + 2 * w2]

    def my_cols(i):
        full = small_nat[:, offs[i] : offs[i + 1]].reshape(-1)
        return cut(full, q, full.shape[0] // Q, 0)

    value_cols, inner_cols, outer_cols, up_cols = [my_cols(i) for i in range(4)]
    out_cols = [small_ring[k][:, offs[4] : offs[5]].reshape(-1) for k in range(A)]
    down_cols = [small_ring[k][:, offs[5] : offs[6]].reshape(-1) for k in range(A)]

    def add_rows(acts, chains):
        width = acts.shape[1] // F
        total = None
        for k in range(A):
            for dy in range(B):
                shard = ((z - k) % A) * B + (y - dy) % B
                part = dot(cut(acts, shard, width, 1), chains[dy][k])
                total = part if total is None else total + part
        return total

    upper3 = add_rows(normed, vio)
    C = upper3.shape[1] // 3
    value, inner, outer = upper3[:, :C], upper3[:, C : 2 * C], upper3[:, 2 * C :]
    taps = cut(conv_taps, q, C, 1)
    gated = (inner * inner_cols * (value * value_cols)).reshape(N, Q, rows, C)
    befores, afters = [], []
    for dc in range(N):
        h = (c - dc) % N
        first = jnp.where(h == 0, 0.0, gated[(dc + 1) % N, :, -1:])
        last = jnp.where(h == N - 1, 0.0, gated[(dc - 1) % N, :, :1])
        befores.append(jnp.concatenate([first, gated[dc, :, :-1]], axis=1))
        afters.append(jnp.concatenate([gated[dc, :, 1:], last], axis=1))
    before, after = jnp.stack(befores), jnp.stack(afters)
    conv = taps[0] * before + taps[1] * gated + taps[2] * after
    hidden = (outer * outer_cols * conv.reshape(-1, C)).astype(bf16)

    def collect(acts, pieces):
        part = jnp.concatenate([dot(acts, p).astype(bf16) for p in pieces], axis=1)
        part = part.reshape(N, Q, rows, -1)
        if N > 2:
            part = jnp.take(part, (c - jnp.arange(N)) % N, axis=0)
            total = lax.psum_scatter(part.astype(f32), "tp", scatter_dimension=0)
        else:
            total = sum([part[0].astype(f32)] + [to_core(part[1], -1).astype(f32)] * (N - 1))
        own = total[0]
        sent = total.astype(bf16)
        for j in range(1, Q):
            dr, dy = peers[j]
            own = own + to_peer(sent[j], -dr, -dy).astype(f32)
        return own

    out_chains = gather_natural(out_weight, 0)
    up_chains = gather_relative([up_weight], 1)
    down_chains = gather_natural(down_weight, 0)

    W = D // A
    middle = []
    for k in range(A):
        mix = collect(hidden, [out_chains[j][k] for j in range(B)])
        middle.append(cut(start_rows, (z - k) % A, W, 1) + mix * out_cols[k])
    square = sum(jnp.sum(m * m, axis=-1, keepdims=True) for m in middle)
    inv = lax.rsqrt(square / D + norm_eps)
    mid_own = jnp.concatenate(
        [(middle[k] * inv * cut(mlp_gain, (z - k) % A, W, 0)).astype(bf16) for k in range(A)],
        axis=1,
    )
    normed_mid = spread(mid_own)

    def add_rows_rel(acts, chains):
        width = acts.shape[1] // F
        total = None
        for k in range(A):
            for dy in range(B):
                shard = k * B + (y - dy) % B
                part = dot(cut(acts, shard, width, 1), chains[dy][k])
                total = part if total is None else total + part
        return total

    upper = add_rows_rel(normed_mid, up_chains)
    act = jnp.square(jax.nn.relu(upper * up_cols)).astype(bf16)
    result = jnp.zeros((T, D), bf16)
    for k in range(A):
        mlp = collect(act, [down_chains[j][k] for j in range(B)])
        piece = (middle[k] + mlp * down_cols[k]).astype(bf16)
        if N > 2:
            blocks = [(0, lax.all_gather(piece, "tp", axis=0, tiled=True))]
        else:
            blocks = [(((c - dc) % N) * rows, to_core(piece, dc) if dc else piece) for dc in range(N)]
        for at, block in blocks:
            result = lax.dynamic_update_slice(result, block, (at, ((z - k) % A) * W))
    return result[None]


def solution(mesh):
    placed = (
        P(("rep", "fs"), None, None),
        P(),
        P("fs", "tp"),
        P(("tp", "fs")),
        P("fs", "tp"),
        P(("tp", "fs")),
        P("fs", "tp"),
        P(("tp", "fs")),
        P(None, "tp"),
        P("tp", "fs"),
        P("fs"),
        P(),
        P("fs", "tp"),
        P(("tp", "fs")),
        P("tp", "fs"),
        P("fs"),
    )
    return jax.shard_map(
        body, mesh=mesh, in_specs=placed, out_specs=P(("rep", "fs"), None, None), check_vma=False
    )
```

```python
import jax
import jax.numpy as jnp
from jax import lax
from jax.experimental import pallas as pl
from jax.experimental.pallas import tpu as pltpu
from jax.sharding import PartitionSpec as P

norm_eps = 1e-06
bf16 = jnp.bfloat16
f32 = jnp.float32


def normalize(values, gain):
    return values * lax.rsqrt(jnp.mean(values * values, axis=-1, keepdims=True) + norm_eps) * gain


def dot(left, right):
    return jnp.dot(left, right, preferred_element_type=f32)


def cut(array, index, width, axis):
    return lax.dynamic_slice_in_dim(array, index * width, width, axis)


VMEM_LIMIT = 60000 * 1024
ANY = pl.BlockSpec(memory_space=pl.ANY)
FULL = pl.BlockSpec(memory_space=pltpu.VMEM)
SCALARS = pl.BlockSpec(memory_space=pltpu.SMEM)


def copies(pairs, sems):
    made = [pltpu.make_async_copy(src, dst, sems.at[i]) for i, (src, dst) in enumerate(pairs)]
    for one in made:
        one.start()
    return made


def mixer_hidden(places, xs, weights, scales, taps, N, Q):
    rows, D = xs[0].shape
    P_, C = len(weights), scales.shape[1]
    wide = weights[0].shape[1]
    T = N * rows

    def kernel(places_ref, scales_ref, taps_ref, *refs):
        x_refs, w_refs = refs[: N * Q], refs[N * Q : N * Q + P_]
        out_ref, x_scr, w_scr, x_sems, w_sems = refs[N * Q + P_ :]
        step = D // P_
        w_copies = copies(
            [
                (w_refs[i], w_scr.at[pl.ds(pl.multiple_of(places_ref[1 + i] * step, step), step), :])
                for i in range(P_)
            ],
            w_sems,
        )
        x_copies = copies(
            [
                (x_refs[dc * Q + j], x_scr.at[j, dc * rows : (dc + 1) * rows, :])
                for j in range(Q)
                for dc in range(N)
            ],
            x_sems,
        )
        core = places_ref[0]
        for one in w_copies:
            one.wait()
        for one in x_copies:
            one.wait()

        def one_sequence(j, carry):
            u = dot(x_scr[j], w_scr[...])
            value = u[:, :C] * scales_ref[0:1, :]
            inner = u[:, C : 2 * C] * scales_ref[1:2, :]
            outer = u[:, 2 * C : 3 * C] * scales_ref[2:3, :]
            gated = inner * value
            row = lax.broadcasted_iota(jnp.int32, (rows, C), 0)
            for dc in range(N):
                h = lax.rem(core - dc + N, N)
                g = gated[dc * rows : (dc + 1) * rows]
                prev_at = ((dc + 1) % N) * rows + rows - 1
                next_at = ((dc - 1) % N) * rows
                first = jnp.where(h == 0, 0.0, gated[prev_at : prev_at + 1])
                last = jnp.where(h == N - 1, 0.0, gated[next_at : next_at + 1])
                before = jnp.where(row == 0, first, pltpu.roll(g, 1, 0))
                after = jnp.where(row == rows - 1, last, pltpu.roll(g, rows - 1, 0))
                conv = taps_ref[0:1, :] * before + taps_ref[1:2, :] * g + taps_ref[2:3, :] * after
                out_ref[dc, j] = (outer[dc * rows : (dc + 1) * rows] * conv).astype(bf16)
            return carry

        lax.fori_loop(0, Q, one_sequence, 0)

    return pl.pallas_call(
        kernel,
        out_shape=jax.ShapeDtypeStruct((N, Q, rows, C), bf16),
        in_specs=[SCALARS, FULL, FULL] + [ANY] * (N * Q + P_),
        out_specs=FULL,
        scratch_shapes=[
            pltpu.VMEM((Q, T, D), bf16),
            pltpu.VMEM((D, wide), bf16),
            pltpu.SemaphoreType.DMA((N * Q,)),
            pltpu.SemaphoreType.DMA((P_,)),
        ],
        compiler_params=pltpu.CompilerParams(vmem_limit_bytes=VMEM_LIMIT),
        name="mixer_hidden",
    )(places, scales, taps, *xs, *weights)


def feed_up(places, xs, weights, cols, inverse, N, Q):
    rows = xs[0][0].shape[0]
    spans = [x.shape[1] for x in xs[0]]
    D = sum(spans)
    P_, C = len(weights), weights[0].shape[1]
    T = N * rows
    flat = [x for piece in xs for x in piece]
    n = len(flat)

    def kernel(places_ref, cols_ref, inverse_ref, *refs):
        x_refs, w_refs = refs[:n], refs[n : n + P_]
        out_ref, x_scr, w_scr, x_sems, w_sems = refs[n + P_ :]
        step = D // P_
        w_copies = copies(
            [
                (w_refs[i], w_scr.at[pl.ds(pl.multiple_of(places_ref[1 + i] * step, step), step), :])
                for i in range(P_)
            ],
            w_sems,
        )
        pairs = []
        for j in range(Q):
            for dc in range(N):
                at = 0
                for i, span in enumerate(spans):
                    pairs.append(
                        (
                            x_refs[(dc * Q + j) * len(spans) + i],
                            x_scr.at[j, dc * rows : (dc + 1) * rows, at : at + span],
                        )
                    )
                    at += span
        x_copies = copies(pairs, x_sems)
        for one in w_copies:
            one.wait()
        for one in x_copies:
            one.wait()

        def one_sequence(j, carry):
            x = x_scr[j]
            plain = x.astype(f32) * inverse_ref[...]
            scale = lax.rsqrt(jnp.mean(plain * plain, axis=-1, keepdims=True) + norm_eps)
            u = jnp.maximum(dot(x, w_scr[...]) * scale * cols_ref[...], 0.0)
            act = (u * u).astype(bf16)
            for dc in range(N):
                out_ref[dc, j] = act[dc * rows : (dc + 1) * rows]
            return carry

        lax.fori_loop(0, Q, one_sequence, 0)

    return pl.pallas_call(
        kernel,
        out_shape=jax.ShapeDtypeStruct((N, Q, rows, C), bf16),
        in_specs=[SCALARS, FULL, FULL] + [ANY] * (n + P_),
        out_specs=FULL,
        scratch_shapes=[
            pltpu.VMEM((Q, T, D), bf16),
            pltpu.VMEM((D, C), bf16),
            pltpu.SemaphoreType.DMA((n,)),
            pltpu.SemaphoreType.DMA((P_,)),
        ],
        compiler_params=pltpu.CompilerParams(vmem_limit_bytes=VMEM_LIMIT),
        name="feed_up",
    )(places, cols, inverse, *flat, *weights)


def project(acts, pieces):
    N, Q, rows, K = acts.shape
    step = pieces[0].shape[1]
    wide = step * len(pieces)

    def kernel(acts_ref, *refs):
        p_refs, outs = refs[: len(pieces)], refs[len(pieces) :]
        for dc in range(N):
            left = acts_ref[dc].reshape(Q * rows, K)
            for i, p in enumerate(p_refs):
                part = dot(left, p[...]).astype(bf16)
                outs[dc][:, :, i * step : (i + 1) * step] = part.reshape(Q, rows, step)

    return pl.pallas_call(
        kernel,
        out_shape=[jax.ShapeDtypeStruct((Q, rows, wide), bf16) for _ in range(N)],
        in_specs=[FULL] * (1 + len(pieces)),
        out_specs=[FULL] * N,
        compiler_params=pltpu.CompilerParams(vmem_limit_bytes=VMEM_LIMIT),
        name="project",
    )(acts, *pieces)


def merge(parts):
    Q, rows, wide = parts[0].shape

    def kernel(*refs):
        ins, outs = refs[: len(parts)], refs[len(parts) :]
        for j in range(Q):
            total = ins[0][j].astype(f32)
            for one in ins[1:]:
                total = total + one[j].astype(f32)
            outs[j][...] = total.astype(outs[j].dtype)

    kinds = [f32] + [bf16] * (Q - 1)
    return pl.pallas_call(
        kernel,
        out_shape=[jax.ShapeDtypeStruct((rows, wide), kind) for kind in kinds],
        in_specs=[FULL] * len(parts),
        out_specs=[FULL] * Q,
        compiler_params=pltpu.CompilerParams(vmem_limit_bytes=VMEM_LIMIT),
        name="merge",
    )(*parts)


def body(
    tokens,
    mix_gain,
    value_weight,
    value_scale,
    inner_weight,
    inner_scale,
    outer_weight,
    outer_scale,
    conv_taps,
    out_weight,
    out_scale,
    mlp_gain,
    up_weight,
    up_scale,
    down_weight,
    down_scale,
):
    R, F, N = lax.axis_size("rep"), lax.axis_size("fs"), lax.axis_size("tp")
    B = 2
    A = F // B
    r, f, c = lax.axis_index("rep"), lax.axis_index("fs"), lax.axis_index("tp")
    z, y = f // B, f % B
    q = r * B + y
    Q = R * B
    T, D = tokens.shape[1:]
    rows = T // N
    peers = [(dr, dy) for dr in range(R) for dy in range(B)]

    def fs_perm(dz, dy):
        return [(i, ((i // B + dz) % A) * B + (i % B + dy) % B) for i in range(F)]

    def to_fs(array, dz, dy):
        return lax.ppermute(array, "fs", fs_perm(dz, dy))

    def to_peer(array, dr, dy):
        perm = [
            (k * F + i, ((k + dr) % R) * F + (i // B) * B + (i % B + dy) % B)
            for k in range(R)
            for i in range(F)
        ]
        return lax.ppermute(array, ("rep", "fs"), perm)

    def to_core(array, dc):
        return lax.ppermute(array, "tp", [(i, (i + dc) % N) for i in range(N)])


    def after(gate, *arrays):
        return lax.optimization_barrier((tuple(gate), arrays))[1]

    def shifts(pieces):
        near = [to_fs(p, 1, 0) for p in pieces]
        far = [to_fs(p, -1, 0) for p in pieces] if A > 2 else []
        return near, far

    def rest(pieces, near, far):
        chains = []
        for i, piece in enumerate(pieces):
            chain = [piece] + [None] * (A - 1)
            chain[1] = near[i]
            if A > 2:
                chain[A - 1] = far[i]
            for k in range(2, A // 2 + 1):
                chain[k] = to_fs(chain[k - 1], 1, 0)
            for k in range(A - 2, A // 2, -1):
                chain[k] = to_fs(chain[k + 1], -1, 0)
            chains.append(chain)
        return chains

    def quarter(weights, axis, dy):
        index = r * B + (y + dy) % B
        parts = [cut(w, index, w.shape[axis] // Q, axis) for w in weights]
        return jnp.concatenate(parts, axis=1).astype(bf16)

    def relative(weights, axis):
        return [
            quarter(weights, axis, 0) if dy == 0 else to_fs(quarter(weights, axis, dy), 0, dy)
            for dy in range(B)
        ]

    def natural(weight, axis):
        mine = relative([weight], axis)
        pieces = []
        for j in range(B):
            piece = mine[0]
            for dy in range(1, B):
                piece = jnp.where((y - dy) % B == j, mine[dy], piece)
            pieces.append(piece)
        return pieces

    def spread_peers(own):
        return [own if j == 0 else to_peer(own, *peers[j]) for j in range(Q)]

    def spread_cores(seqs):
        if N > 2:
            every = lax.all_gather(jnp.stack(seqs), "tp", axis=0)
            every = jnp.take(every, (c - jnp.arange(N)) % N, axis=0)
            return [every[dc, j] for dc in range(N) for j in range(Q)]
        return seqs + [to_core(s, dc) for dc in range(1, N) for s in seqs]

    def join_cores(parts):
        if N > 2:
            part = jnp.take(jnp.stack(parts), (c - jnp.arange(N)) % N, axis=0)
            return [lax.psum_scatter(part.astype(f32), "tp", scatter_dimension=0).astype(bf16)]
        return [parts[0]] + [to_core(parts[dc], -dc) for dc in range(1, N)]

    def reduce_peers(merged):
        return [to_peer(merged[j], -peers[j][0], -peers[j][1]) for j in range(1, Q)]

    def add_all(merged, received):
        total = merged[0]
        for one in received:
            total = total + one.astype(f32)
        return total

    W = D // A
    places_nat = jnp.stack(
        [c] + [((z - k) % A) * B + (y - dy) % B for dy in range(B) for k in range(A)]
    ).astype(jnp.int32)
    places_rel = jnp.stack(
        [c] + [k * B + (y - dy) % B for dy in range(B) for k in range(A)]
    ).astype(jnp.int32)

    vio = relative([value_weight, inner_weight, outer_weight], 1)
    vio_near, vio_far = shifts(vio)

    start_rows = cut(tokens[0], c, rows, 0).astype(f32)
    normed_own = normalize(start_rows, mix_gain).astype(bf16)
    normed = spread_cores(spread_peers(normed_own))

    smalls = jnp.concatenate(
        [value_scale, inner_scale, outer_scale, up_scale, out_scale, down_scale]
    )
    small_set = jnp.stack([smalls] + [to_fs(smalls, 0, dy) for dy in range(1, B)])
    small_set = jnp.take(small_set, (y - jnp.arange(B)) % B, axis=0)
    s_near, s_far = shifts([small_set])
    small_ring = jnp.stack(rest([small_set], s_near, s_far)[0])
    small_nat = jnp.take(small_ring, (z - jnp.arange(A)) % A, axis=0).reshape(F, -1)
    w0, w1, w2 = value_scale.shape[0], up_scale.shape[0], out_scale.shape[0]
    offs = [0, w0, 2 * w0, 3 * w0, 3 * w0 + w1, 3 * w0 + w1 + w2, 3 * w0 + w1 + 2 * w2]

    def my_cols(i):
        full = small_nat[:, offs[i] : offs[i + 1]].reshape(1, -1)
        return cut(full, q, full.shape[1] // Q, 1)

    vio_cols = jnp.concatenate([my_cols(i) for i in range(3)], axis=0)
    up_cols = my_cols(3)
    out_cols = [small_ring[k][:, offs[4] : offs[5]].reshape(1, -1) for k in range(A)]
    down_cols = [small_ring[k][:, offs[5] : offs[6]].reshape(1, -1) for k in range(A)]
    C = vio_cols.shape[1]
    taps = cut(conv_taps, q, C, 1)

    vio_chains = rest(vio, vio_near, vio_far)
    out = natural(out_weight, 0)
    out = list(after(vio_near, *out))
    out_near, out_far = shifts(out)
    out_chains = rest(out, out_near, out_far)
    up = relative([up_weight], 1)
    up = list(after(vio_far + out_near, *up))
    up_near, up_far = shifts(up)
    up_chains = rest(up, up_near, up_far)
    down = natural(down_weight, 0)
    down = list(after(up_near, *down))
    down_near, down_far = shifts(down)
    down_chains = rest(down, down_near, down_far)

    hidden = mixer_hidden(
        places_nat, normed, [w for chain in vio_chains for w in chain], vio_cols, taps, N, Q
    )

    order = [0, 1, A - 1] + [k for k in range(2, A - 1)] if A > 2 else list(range(A))
    middle, sent = {}, {}
    for k in order:
        merged = merge(join_cores(project(hidden, [out_chains[j][k] for j in range(B)])))
        mix = add_all(merged, reduce_peers(merged))
        at = (z - k) % A
        middle[k] = cut(start_rows, at, W, 1) + mix * out_cols[k]
        own = (middle[k] * cut(mlp_gain, at, W, 0)).astype(bf16)
        sent[k] = spread_cores(spread_peers(own))
    xs = [[sent[k][i] for k in range(A)] for i in range(N * Q)]
    inverse = jnp.concatenate([cut(1.0 / mlp_gain, (z - k) % A, W, 0) for k in range(A)])[None]
    act = feed_up(places_rel, xs, [w for chain in up_chains for w in chain], up_cols, inverse, N, Q)

    result = jnp.zeros((T, D), bf16)
    for k in order:
        merged = merge(join_cores(project(act, [down_chains[j][k] for j in range(B)])))
        mlp = add_all(merged, reduce_peers(merged))
        piece = (middle[k] + mlp * down_cols[k]).astype(bf16)
        if N > 2:
            blocks = [(0, lax.all_gather(piece, "tp", axis=0, tiled=True))]
        else:
            blocks = [(((c - dc) % N) * rows, to_core(piece, dc) if dc else piece) for dc in range(N)]
        for at, block in blocks:
            result = lax.dynamic_update_slice(result, block, (at, ((z - k) % A) * W))
    return result[None]


def solution(mesh):
    placed = (
        P(("rep", "fs"), None, None),
        P(),
        P("fs", "tp"),
        P(("tp", "fs")),
        P("fs", "tp"),
        P(("tp", "fs")),
        P("fs", "tp"),
        P(("tp", "fs")),
        P(None, "tp"),
        P("tp", "fs"),
        P("fs"),
        P(),
        P("fs", "tp"),
        P(("tp", "fs")),
        P("tp", "fs"),
        P("fs"),
    )
    return jax.shard_map(
        body, mesh=mesh, in_specs=placed, out_specs=P(("rep", "fs"), None, None), check_vma=False
    )
```
